32 devices in a mesh: ep: 16 (over z, y, x), tp: 2 (over core).
Axes of the slice: x: 2, y: 2, z: 4, core: 2. Of those that a mesh axis runs over, the one named last changes fastest.
Arguments:
- tokens: bfloat16 [384, 2048], P('ep'), may hold values from -6 to 6
- attn_gain: float32 [2048], replicated, may hold values from 0.1 to 1.9
- w_query: bfloat16 [2048, 1024], P(None, 'tp'), may hold values from -0.125 to 0.125
- w_key: bfloat16 [2048, 1024], P(None, 'tp'), may hold values from -0.125 to 0.125
- w_value: bfloat16 [2048, 1024], P(None, 'tp'), may hold values from -0.125 to 0.125
- w_zgate: bfloat16 [2048, 1024], P(None, 'tp'), may hold values from -0.125 to 0.125
- w_decay: bfloat16 [2048, 8], P(None, 'tp'), may hold values from -0.125 to 0.125
- w_beta: bfloat16 [2048, 8], P(None, 'tp'), may hold values from -0.125 to 0.125
- decay_rate: float32 [8], P('tp'), may hold values from 0.05 to 2
- decay_bias: float32 [8], P('tp'), may hold values from -3 to 3
- state: float32 [384, 8, 128, 128], P('ep', 'tp'), may hold values from -2 to 2
- out_gain: float32 [128], replicated, may hold values from 0.1 to 1.9
- w_out: bfloat16 [1024, 2048], P('tp'), may hold values from -0.1875 to 0.1875
- ffn_gain: float32 [2048], replicated, may hold values from 0.1 to 1.9
- expert_gate: bfloat16 [16, 2048, 512], P('ep', None, 'tp'), may hold values from -0.125 to 0.125
- expert_up: bfloat16 [16, 2048, 512], P('ep', None, 'tp'), may hold values from -0.125 to 0.125
- expert_down: bfloat16 [16, 512, 2048], P('ep', 'tp'), may hold values from -0.25 to 0.25
- routes: int32 [384, 2], P('ep'), may hold values from 0 to 15, all different within a row; in each aligned block of 24 rows (0 to 23, 24 to 47, ...) at most 6 rows name the same one
- route_weight: float32 [384, 2], P('ep'), may hold values from 0.2 to 1
Outputs:
- layer_out: bfloat16 [384, 2048], P('ep', 'tp')
- new_state: float32 [384, 8, 128, 128], P('ep', 'tp')
The draws below stay inside these ranges and needn't reach their ends.
Inputs may be any that keep to these rules, and one draw needn't show every extreme that they name: `routes`: the 2 entries of a row differ. Among the rows of one index of ep (aligned blocks of 24 rows) no expert is named more than 6 times, a bound that some block reaches.
All inputs are finite; a program needn't handle non-finite values.
Results may differ from the reference program's by a relative error of at most 0.014.
Values may be sent and summed in bfloat16 or wider, within the bound.
A program may use at most 128 MiB of HBM per device.

```python
import math
import jax
import jax.numpy as jnp
import numpy as np
from jax import lax

D = 2048
HEADS = 8
HEAD_DIM = 128
FF_EXP = 512
TOP_K = 2
SEQS_DEV = 24
SEQS = 384
EXPERTS = 16
CAP = 6
N_EP = 16
N_TP = 2


def levels(stream_key, shape, cuts, least, top_value):
    def one(position, blocks):
        draws = jax.random.uniform(jax.random.fold_in(jax.random.fold_in(stream_key, 6), position), (blocks,), jnp.float32, least / len(cuts), top_value / len(cuts))
        return jnp.repeat(jnp.exp(draws), shape[position] // blocks).reshape((-1,) + (1,) * (len(shape) - position - 1))

    factor_of = one(*cuts[0])
    for cut in cuts[1:]:
        factor_of = factor_of * one(*cut)
    return factor_of


def deal_out(rng, own, number, rows, count, top, reach, lean):
    sequence = jax.random.permutation(rng, count)
    heavy_load, ordinary = shares(count, rows * top, reach, lean, True), shares(count, rows * top, reach, lean, False)
    places = jnp.arange(count)

    def named(tallies, rotation):
        used = int((tallies > 0).sum())
        fixed = max(1, used // 4)
        moved = fixed + (places - fixed + rotation * (used - fixed)) % max(1, count - fixed)
        return jnp.zeros((count,), jnp.int32).at[sequence[jnp.where(places < fixed, places, moved)]].set(jnp.asarray(tallies, jnp.int32))

    tallies = jnp.where(number % 4 == 0, named(heavy_load, number // 4), named(ordinary, number - number // 4 - 1))
    mixed = jax.random.permutation(jax.random.fold_in(own, 3), count)
    giver, sink = mixed[0:count // 2 * 2:2], mixed[1:count // 2 * 2:2]
    slack = jnp.minimum(tallies[giver] - 1, reach - tallies[sink]) // 2
    slack = jnp.where((giver == sequence[0]) | (sink == sequence[0]) | (tallies[sink] == 0), 0, jnp.maximum(slack, 0))
    moved = jax.random.randint(jax.random.fold_in(own, 4), (count // 2,), 0, 1 << 20) % (slack + 1)
    tallies = tallies.at[giver].add(-moved).at[sink].add(moved)
    items = jnp.searchsorted(jnp.cumsum(tallies), jnp.arange(rows * top), side="right").astype(jnp.int32)
    listing = items.reshape(top, rows).T
    listing = listing[jax.random.permutation(jax.random.fold_in(own, 1), rows)]
    rotation = jax.random.randint(jax.random.fold_in(own, 2), (rows, 1), 0, top)
    return jnp.take_along_axis(listing, (jnp.arange(top)[None, :] + rotation) % top, axis=1)


def shares(amount, total, reach, slope, full):
    weights = [(1 << 20) // math.isqrt(rank ** slope) + 1 for rank in range(1, amount + 1)]
    largest = reach if full else min(reach, max(-(-total // amount), total * weights[0] // sum(weights)))
    least = 1 if total - largest >= amount - 1 else 0
    counts, rest = [largest] + [least] * (amount - 1), total - largest - least * (amount - 1)
    while rest > 0:
        movable = [i for i in range(1, amount) if counts[i] < largest] or [i for i in range(1, amount) if counts[i] < reach]
        pool, budget = sum([weights[i] for i in movable]), rest
        for i in movable:
            extra = min(reach - counts[i], max(1, budget * weights[i] // pool), rest)
            counts[i] = counts[i] + extra
            rest = rest - extra
    return np.array(counts)


def normal_values(stream_key, dims, width, limit, shards=(), kind=jnp.bfloat16):
    entries = width * jax.random.normal(stream_key, dims, jnp.float32)
    if shards:
        entries = entries * levels(stream_key, dims, shards, -0.22, 0.18)
    return jnp.clip(entries, -limit, limit).astype(kind)


def setup_inputs(seed: int = 0) -> dict:
    streams_of = jax.random.split(jax.random.key(seed), 20)
    tokens = normal_values(streams_of[0], (SEQS, D), 1.0, 6.0, ((0, 16),))
    attn_gain = jnp.clip(1.0 + 0.18 * jax.random.normal(streams_of[1], (D,), jnp.float32), 0.1, 1.9)
    w_query = normal_values(streams_of[2], (D, HEADS * HEAD_DIM), D ** -0.5, 0.125, ((1, 2),))
    w_key = normal_values(streams_of[3], (D, HEADS * HEAD_DIM), D ** -0.5, 0.125, ((1, 2),))
    w_value = normal_values(streams_of[4], (D, HEADS * HEAD_DIM), D ** -0.5, 0.125, ((1, 2),))
    w_zgate = normal_values(streams_of[5], (D, HEADS * HEAD_DIM), D ** -0.5, 0.125, ((1, 2),))
    w_decay = normal_values(streams_of[6], (D, HEADS), D ** -0.5, 0.125, ((1, 2),))
    w_beta = normal_values(streams_of[7], (D, HEADS), D ** -0.5, 0.125, ((1, 2),))
    decay_rate = jnp.clip(jnp.exp(math.log(2.0) - 3.6888794 * jax.random.uniform(streams_of[8], (HEADS,), jnp.float32) ** levels(streams_of[8], (HEADS,), ((0, 2),), -0.2, 0.2)), 0.05, 2.0)
    decay_bias = normal_values(streams_of[9], (HEADS,), 1.0, 3.0, ((0, 2),), jnp.float32)
    state = normal_values(streams_of[10], (SEQS, HEADS, HEAD_DIM, HEAD_DIM), 0.3, 2.0, ((0, 16), (1, 2)), jnp.float32)
    out_gain = jnp.clip(1.0 + 0.18 * jax.random.normal(streams_of[11], (HEAD_DIM,), jnp.float32), 0.1, 1.9)
    w_out = normal_values(streams_of[12], (HEADS * HEAD_DIM, D), (HEADS * HEAD_DIM) ** -0.5, 0.1875, ((0, 2),))
    ffn_gain = jnp.clip(1.0 + 0.18 * jax.random.normal(streams_of[13], (D,), jnp.float32), 0.1, 1.9)
    expert_gate = normal_values(streams_of[14], (EXPERTS, D, FF_EXP), D ** -0.5, 0.125, ((0, 16), (2, 2)))
    expert_up = normal_values(streams_of[15], (EXPERTS, D, FF_EXP), D ** -0.5, 0.125, ((0, 16), (2, 2)))
    expert_down = normal_values(streams_of[16], (EXPERTS, FF_EXP, D), FF_EXP ** -0.5, 0.25, ((0, 16), (1, 2)))
    routes_keys = jax.random.split(jax.random.fold_in(streams_of[17], 1), SEQS // SEQS_DEV)
    routes_turns = jax.random.permutation(jax.random.fold_in(streams_of[17], 3), SEQS // SEQS_DEV)
    routes = jax.vmap(lambda own, number: deal_out(jax.random.fold_in(streams_of[17], 2), own, number, SEQS_DEV, EXPERTS, TOP_K, CAP, 2))(routes_keys, routes_turns).reshape((SEQS, TOP_K))
    route_weight = jnp.clip(0.2 + 0.8 * jax.random.uniform(streams_of[18], (SEQS, TOP_K), jnp.float32) ** levels(streams_of[18], (SEQS, TOP_K), ((0, 16),), -0.2, 0.2), 0.2, 1.0)
    return dict(tokens=tokens, attn_gain=attn_gain, w_query=w_query, w_key=w_key, w_value=w_value, w_zgate=w_zgate, w_decay=w_decay, w_beta=w_beta, decay_rate=decay_rate, decay_bias=decay_bias, state=state, out_gain=out_gain, w_out=w_out, ffn_gain=ffn_gain, expert_gate=expert_gate, expert_up=expert_up, expert_down=expert_down, routes=routes, route_weight=route_weight)


EPS = 1e-06

def rms_scale(rows, gain):
    return rows * lax.rsqrt(lax.optimization_barrier(jnp.mean(rows * rows, axis=-1, keepdims=True)) + EPS) * gain

def unit_rows(rows):
    return rows * lax.rsqrt(lax.optimization_barrier(jnp.sum(rows * rows, axis=-1, keepdims=True)) + EPS)

def mixer_block(args):
    normed, w_query, w_key, w_value, w_zgate, w_decay, w_beta, decay_rate, decay_bias, state, out_gain = args
    seqs = normed.shape[0]

    def project(weight):
        return jnp.dot(normed, weight, preferred_element_type=jnp.float32).astype(jnp.bfloat16)

    def heads_of(raw):
        return raw.reshape(seqs, HEADS, HEAD_DIM).astype(jnp.float32)
    query = unit_rows(jax.nn.silu(heads_of(project(w_query)))) * HEAD_DIM ** (-0.5)
    key = unit_rows(jax.nn.silu(heads_of(project(w_key))))
    value = jax.nn.silu(heads_of(project(w_value)))
    zmul = jax.nn.silu(heads_of(project(w_zgate)))
    fade = jnp.exp(-decay_rate * jax.nn.softplus(project(w_decay).astype(jnp.float32) + decay_bias))
    beta = jax.nn.sigmoid(project(w_beta).astype(jnp.float32))
    predicted = jnp.einsum('shkv,shk->shv', state, key, precision=lax.Precision.HIGHEST)
    written = beta[..., None] * (value - fade[..., None] * predicted)
    updated = fade[..., None, None] * state + key[..., :, None] * written[..., None, :]
    read = jnp.einsum('shkv,shk->shv', updated, query, precision=lax.Precision.HIGHEST)
    heads_out = (rms_scale(read, out_gain) * zmul).astype(jnp.bfloat16)
    return (heads_out.reshape(seqs, HEADS * HEAD_DIM), updated)

def reference(tokens, attn_gain, w_query, w_key, w_value, w_zgate, w_decay, w_beta, decay_rate, decay_bias, state, out_gain, w_out, ffn_gain, expert_gate, expert_up, expert_down, routes, route_weight):
    resid_in = tokens.astype(jnp.float32)
    normed = rms_scale(resid_in, attn_gain).astype(jnp.bfloat16)

    def one_block(args):
        block_rows, block_state = args
        return mixer_block((block_rows, w_query, w_key, w_value, w_zgate, w_decay, w_beta, decay_rate, decay_bias, block_state, out_gain))
    heads_out, new_state = lax.map(one_block, (normed.reshape(N_EP, SEQS_DEV, D), state.reshape(N_EP, SEQS_DEV, HEADS, HEAD_DIM, HEAD_DIM)))
    heads_out = heads_out.reshape(SEQS, HEADS * HEAD_DIM)
    new_state = new_state.reshape(SEQS, HEADS, HEAD_DIM, HEAD_DIM)
    group = HEADS * HEAD_DIM // N_TP
    mixed = jnp.zeros((SEQS, D), jnp.float32)
    for part in range(N_TP):
        term = jnp.dot(heads_out[:, part * group:(part + 1) * group], w_out[part * group:(part + 1) * group], preferred_element_type=jnp.float32)
        mixed = mixed + term.astype(jnp.bfloat16).astype(jnp.float32)
    resid = resid_in + mixed
    moe_in = rms_scale(resid, ffn_gain).astype(jnp.bfloat16)
    flat = routes.reshape(N_EP, SEQS_DEV * TOP_K)
    onehot = (flat[..., None] == jnp.arange(EXPERTS, dtype=jnp.int32)[None, None, :]).astype(jnp.int32)
    before = jnp.cumsum(onehot, axis=1) - onehot
    slot = lax.optimization_barrier(jnp.sum(before * onehot, axis=-1)).astype(jnp.int32)
    block_ids = jnp.broadcast_to(jnp.arange(N_EP, dtype=jnp.int32)[:, None], flat.shape)
    row_of = (jnp.arange(SEQS_DEV * TOP_K, dtype=jnp.int32) // TOP_K)[None, :] + SEQS_DEV * block_ids
    table = jnp.zeros((EXPERTS, N_EP, CAP), jnp.int32).at[flat, block_ids, slot].set(row_of.astype(jnp.int32))
    piece = FF_EXP // N_TP

    def run_expert(args):
        w_gate, w_up, w_down, picks = args
        rows = moe_in[picks.reshape(-1)]
        gate = jnp.dot(rows, w_gate, preferred_element_type=jnp.float32)
        up = jnp.dot(rows, w_up, preferred_element_type=jnp.float32)
        hidden = (jax.nn.silu(gate) * up).astype(jnp.bfloat16)
        total = jnp.zeros((rows.shape[0], D), jnp.float32)
        for part in range(N_TP):
            term = jnp.dot(hidden[:, part * piece:(part + 1) * piece], w_down[part * piece:(part + 1) * piece], preferred_element_type=jnp.float32)
            total = total + term.astype(jnp.bfloat16).astype(jnp.float32)
        return total.astype(jnp.bfloat16).reshape(N_EP, CAP, D)
    results = lax.map(run_expert, (expert_gate, expert_up, expert_down, table))
    per_route = results[flat, block_ids, slot].astype(jnp.float32).reshape(SEQS, TOP_K, D)
    combined = lax.optimization_barrier(jnp.sum(per_route * route_weight[..., None], axis=1))
    layer_out = (resid + combined).astype(jnp.bfloat16)
    return (layer_out, new_state)
```

```python
import functools

import jax
import jax.numpy as jnp
from jax import lax
from jax.experimental import pallas as pl
from jax.experimental.pallas import tpu as pltpu
from jax.sharding import PartitionSpec as P

EPS = 1e-06
F32 = jnp.float32
BF16 = jnp.bfloat16
ANY = pl.BlockSpec(memory_space=pl.ANY)
VMEM = pl.BlockSpec(memory_space=pltpu.VMEM)


def rms_scale(rows, gain):
    return rows * lax.rsqrt(jnp.mean(rows * rows, axis=-1, keepdims=True) + EPS) * gain


def unit_rows(rows):
    return rows * lax.rsqrt(jnp.sum(rows * rows, axis=-1, keepdims=True) + EPS)


def silu(x):
    return x * jax.nn.sigmoid(x)


def mixer_kernel(
    step,
    tokens,
    gain,
    wq,
    wk,
    wv,
    wz,
    wd,
    wb,
    rate,
    bias,
    state,
    out_gain,
    heads_out,
    new_state,
    wbuf,
    st,
    ns,
    kq,
    vals,
    zbuf,
    fades,
    betas,
    dots,
    reads,
    w_sem,
    in_sem,
    out_sem,
):
    seqs, heads, dim, _ = st.shape
    chunks = seqs // step

    def w_copy(n):
        return pltpu.make_async_copy((wq, wk, wv, wz)[n], wbuf.at[n], w_sem.at[n])

    def in_copy(c):
        rows = pl.ds(c * step, step)
        return pltpu.make_async_copy(state.at[rows], st.at[rows], in_sem.at[c])

    def out_copy(c):
        rows = pl.ds(c * step, step)
        return pltpu.make_async_copy(ns.at[rows], new_state.at[rows], out_sem.at[c])

    for n in range(4):
        w_copy(n).start()
    for c in range(chunks):
        in_copy(c).start()

    normed = rms_scale(tokens[...].astype(F32), gain[...]).astype(BF16)

    def rounded(weight):
        return jnp.dot(normed, weight, preferred_element_type=F32).astype(BF16).astype(F32)

    xa = rounded(wd[...]) + bias[...]
    fade = jnp.exp(-rate[...] * (jnp.maximum(xa, 0.0) + jnp.log1p(jnp.exp(-jnp.abs(xa)))))
    beta = jax.nn.sigmoid(rounded(wb[...]))
    for h in range(heads):
        fades[:, h, :] = jnp.broadcast_to(fade[:, h : h + 1], (seqs, dim))
        betas[:, h, :] = jnp.broadcast_to(beta[:, h : h + 1], (seqs, dim))
    w_copy(0).wait()
    raw_q = rounded(wbuf[0])
    w_copy(1).wait()
    raw_k = rounded(wbuf[1])
    for h in range(heads):
        cols = slice(h * dim, (h + 1) * dim)
        query = unit_rows(silu(raw_q[:, cols])) * dim ** (-0.5)
        key = unit_rows(silu(raw_k[:, cols]))
        kq[:, h, :] = key
        kq[:, heads + h, :] = query
        dots[:, h, :] = jnp.broadcast_to(jnp.sum(key * query, axis=-1, keepdims=True), (seqs, dim))
    w_copy(2).wait()
    value = silu(rounded(wbuf[2]))
    for h in range(heads):
        vals[:, h, :] = value[:, h * dim : (h + 1) * dim]
    w_copy(3).wait()
    zbuf[...] = silu(rounded(wbuf[3]))

    def one_chunk(c, carry):
        in_copy(c).wait()
        for i in range(step):
            s = c * step + i
            turned = kq[s].T
            fs, bs, vs, ds = fades[s], betas[s], vals[s], dots[s]
            for h in range(heads):
                block = st[s, h]
                kc = jnp.broadcast_to(turned[:, h : h + 1], (dim, dim))
                qc = jnp.broadcast_to(turned[:, heads + h : heads + h + 1], (dim, dim))
                f = fs[h : h + 1]
                pred = jnp.sum(block * kc, axis=0, keepdims=True)
                proj = jnp.sum(block * qc, axis=0, keepdims=True)
                written = bs[h : h + 1] * (vs[h : h + 1] - f * pred)
                ns[s, h] = f * block + kc * written
                reads[s, pl.ds(h, 1)] = f * proj + written * ds[h : h + 1]
        out_copy(c).start()
        return carry

    lax.fori_loop(0, chunks, one_chunk, 0)
    for h in range(heads):
        cols = slice(h * dim, (h + 1) * dim)
        heads_out[:, cols] = (rms_scale(reads[:, h, :], out_gain[...]) * zbuf[:, cols]).astype(BF16)
    for c in range(chunks):
        out_copy(c).wait()


def expert_kernel(
    n_ep,
    n_tp,
    top,
    cap,
    groups,
    tokens,
    heads_out,
    w_out,
    ffn_gain,
    w_gate,
    w_up,
    w_down,
    routes,
    weights,
    out,
    wo,
    wg,
    wu,
    wdn,
    part_out,
    part_in,
    resid,
    moe,
    disp,
    arrived,
    acc_g,
    acc_u,
    other,
    other_in,
    mine,
    ret_out,
    ret_in,
    w_sem,
    part_sem,
    go_send,
    go_recv,
    fw_send,
    fw_recv,
    half_send,
    half_recv,
    back_send,
    back_recv,
):
    seqs, width = tokens.shape
    cols = width // n_tp
    e = lax.axis_index("ep")
    t = lax.axis_index("tp")
    u = n_tp - 1 - t

    def peer(i):
        return lax.rem(e + i, n_ep)

    def source(i):
        return lax.rem(e + n_ep - i, n_ep)

    partner = {"ep": e, "tp": u}
    mesh_ids = pl.DeviceIdType.MESH
    barrier = pltpu.get_barrier_semaphore()
    pl.semaphore_signal(barrier, inc=1, device_id=partner, device_id_type=mesh_ids)

    def greet(i, carry):
        pl.semaphore_signal(barrier, inc=1, device_id={"ep": peer(i), "tp": t}, device_id_type=mesh_ids)
        return carry

    lax.fori_loop(1, n_ep, greet, 0)

    loads = [
        pltpu.make_async_copy(src, dst, w_sem.at[n])
        for n, (src, dst) in enumerate(
            ((w_out, wo), (w_gate.at[0], wg), (w_up.at[0], wu), (w_down.at[0], wdn))
        )
    ]
    for load in loads:
        load.start()

    lower = (
        lax.broadcasted_iota(jnp.int32, (seqs, seqs), 1)
        < lax.broadcasted_iota(jnp.int32, (seqs, seqs), 0)
    ).astype(BF16)
    picks = []
    taken = jnp.zeros((1, n_ep), F32)
    for j in range(top):
        route = routes[:, j : j + 1]
        hot = lax.broadcasted_iota(jnp.int32, (seqs, n_ep), 1) == route
        hot_f = hot.astype(F32)
        before = jnp.dot(lower, hot_f.astype(BF16), preferred_element_type=F32) + taken
        slot = jnp.sum(before * hot_f, axis=1, keepdims=True).astype(jnp.int32)
        taken = taken + jnp.sum(hot_f, axis=0, keepdims=True)
        place = route * cap + slot
        picks.append(
            (lax.broadcasted_iota(jnp.int32, (seqs, n_ep * cap), 1) == place).astype(F32)
        )
    spread = sum(picks[1:], picks[0]).T.astype(BF16)

    loads[0].wait()
    part_out[...] = jnp.dot(heads_out[...], wo[...], preferred_element_type=F32).astype(BF16)
    pl.semaphore_wait(barrier, n_ep)

    swap = pltpu.make_async_remote_copy(
        src_ref=part_out,
        dst_ref=part_in,
        send_sem=part_sem.at[0],
        recv_sem=part_sem.at[1],
        device_id=partner,
        device_id_type=mesh_ids,
    )
    swap.start()
    swap.wait()
    rows = tokens[...].astype(F32) + (part_out[...].astype(F32) + part_in[...].astype(F32))
    resid[...] = rows
    moe[...] = rms_scale(rows, ffn_gain[...]).astype(BF16)
    own = pl.ds(pl.multiple_of(t * cols, 128), cols)
    far = pl.ds(pl.multiple_of(u * cols, 128), cols)
    going = jnp.dot(spread, moe[:, own], preferred_element_type=F32)
    disp[...] = going.reshape(n_ep, cap, cols).astype(BF16)

    def go(i):
        return pltpu.make_async_remote_copy(
            src_ref=disp.at[peer(i)],
            dst_ref=arrived.at[t, e],
            send_sem=go_send.at[i],
            recv_sem=go_recv.at[i],
            device_id={"ep": peer(i), "tp": t},
            device_id_type=mesh_ids,
        )

    def forward(i):
        s = source(i)
        return pltpu.make_async_remote_copy(
            src_ref=arrived.at[t, s],
            dst_ref=arrived.at[t, s],
            send_sem=fw_send.at[i],
            recv_sem=fw_recv.at[i],
            device_id=partner,
            device_id_type=mesh_ids,
        )

    def go_start(i, carry):
        go(i).start()
        return carry

    lax.fori_loop(1, n_ep, go_start, 0)
    arrived[t, e] = disp[e]
    forward(0).start()

    def pass_on(i, carry):
        go(i).wait_recv()
        forward(i).start()
        return carry

    lax.fori_loop(1, n_ep, pass_on, 0)
    loads[1].wait()
    loads[2].wait()

    def half(which):
        got = arrived[which].astype(F32).reshape(n_ep * cap, cols).astype(BF16)
        part = pl.ds(pl.multiple_of(which * cols, 128), cols)
        return (
            jnp.dot(got, wg[part, :], preferred_element_type=F32),
            jnp.dot(got, wu[part, :], preferred_element_type=F32),
        )

    acc_g[...], acc_u[...] = half(t)

    def fw_done(i, carry):
        forward(i).wait_recv()
        return carry

    lax.fori_loop(0, n_ep, fw_done, 0)
    more_g, more_u = half(u)
    hidden = (silu(acc_g[...] + more_g) * (acc_u[...] + more_u)).astype(BF16)
    loads[3].wait()

    size = n_ep // groups

    def give(g):
        span = pl.ds(g * size, size)
        return pltpu.make_async_remote_copy(
            src_ref=other.at[span],
            dst_ref=other_in.at[span],
            send_sem=half_send.at[g],
            recv_sem=half_recv.at[g],
            device_id=partner,
            device_id_type=mesh_ids,
        )

    def back(s):
        i = lax.rem(e + n_ep - s, n_ep)
        return pltpu.make_async_remote_copy(
            src_ref=ret_out.at[s],
            dst_ref=ret_in.at[e],
            send_sem=back_send.at[i],
            recv_sem=back_recv.at[i],
            device_id={"ep": s, "tp": t},
            device_id_type=mesh_ids,
        )

    for g in range(groups):
        rows_g = hidden[g * size * cap : (g + 1) * size * cap]
        term = jnp.dot(rows_g, wdn[:, far], preferred_element_type=F32)
        other[pl.ds(g * size, size)] = term.reshape(size, cap, cols).astype(BF16)
        give(g).start()
    term = jnp.dot(hidden, wdn[:, own], preferred_element_type=F32)
    mine[...] = term.reshape(n_ep, cap, cols).astype(BF16)
    for g in range(groups):
        span = pl.ds(g * size, size)
        give(g).wait_recv()
        both = mine[span].astype(F32) + other_in[span].astype(F32)
        ret_out[span] = both.astype(BF16)

        def back_start(s, carry):
            @pl.when(s != e)
            def _():
                back(s).start()

            return carry

        lax.fori_loop(g * size, (g + 1) * size, back_start, 0)
    ret_in[e] = ret_out[e]

    def back_done(i, carry):
        back(source(i)).wait_recv()
        return carry

    lax.fori_loop(1, n_ep, back_done, 0)
    returned = ret_in[...].astype(F32).reshape(n_ep * cap, cols).astype(BF16)
    total = resid[:, own]
    combined = None
    for j in range(top):
        found = jnp.dot(picks[j].astype(BF16), returned, preferred_element_type=F32)
        term = found * weights[:, j : j + 1]
        combined = term if combined is None else combined + term
    out[...] = (total + combined).astype(BF16)

    forward(0).wait_send()

    def sent(i, carry):
        go(i).wait_send()
        forward(i).wait_send()
        back(source(i)).wait_send()
        return carry

    lax.fori_loop(1, n_ep, sent, 0)
    for g in range(groups):
        give(g).wait_send()


def per_device(
    n_ep,
    n_tp,
    tokens,
    attn_gain,
    w_query,
    w_key,
    w_value,
    w_zgate,
    w_decay,
    w_beta,
    decay_rate,
    decay_bias,
    state,
    out_gain,
    w_out,
    ffn_gain,
    expert_gate,
    expert_up,
    expert_down,
    routes,
    route_weight,
):
    seqs, width = tokens.shape
    heads, dim = state.shape[1], state.shape[2]
    top = routes.shape[1]
    inner = heads * dim
    step = 2 if seqs % 2 == 0 else 1
    chunks = seqs // step
    heads_out, new_state = pl.pallas_call(
        functools.partial(mixer_kernel, step),
        out_shape=(
            jax.ShapeDtypeStruct((seqs, inner), BF16),
            jax.ShapeDtypeStruct(state.shape, F32),
        ),
        in_specs=[VMEM, VMEM, ANY, ANY, ANY, ANY, VMEM, VMEM, VMEM, VMEM, ANY, VMEM],
        out_specs=(VMEM, ANY),
        scratch_shapes=[
            pltpu.VMEM((4, width, inner), BF16),
            pltpu.VMEM(state.shape, F32),
            pltpu.VMEM(state.shape, F32),
            pltpu.VMEM((seqs, 2 * heads, dim), F32),
            pltpu.VMEM((seqs, heads, dim), F32),
            pltpu.VMEM((seqs, inner), F32),
            pltpu.VMEM((seqs, heads, dim), F32),
            pltpu.VMEM((seqs, heads, dim), F32),
            pltpu.VMEM((seqs, heads, dim), F32),
            pltpu.VMEM((seqs, heads, dim), F32),
            pltpu.SemaphoreType.DMA((4,)),
            pltpu.SemaphoreType.DMA((chunks,)),
            pltpu.SemaphoreType.DMA((chunks,)),
        ],
        compiler_params=pltpu.CompilerParams(vmem_limit_bytes=48 * 1024 * 1024),
        name="mixer",
    )(
        tokens,
        attn_gain.reshape(1, width),
        w_query,
        w_key,
        w_value,
        w_zgate,
        w_decay,
        w_beta,
        decay_rate.reshape(1, heads),
        decay_bias.reshape(1, heads),
        state,
        out_gain.reshape(1, dim),
    )

    cap = -(-max(2, 2 * seqs * top // n_ep) // 8) * 8
    cols = width // n_tp
    ff = expert_gate.shape[2]
    groups = 4 if n_ep % 4 == 0 else 1
    slots = (n_ep, cap, cols)
    dma = pltpu.SemaphoreType.DMA
    layer_out = pl.pallas_call(
        functools.partial(expert_kernel, n_ep, n_tp, top, cap, groups),
        out_shape=jax.ShapeDtypeStruct((seqs, cols), BF16),
        in_specs=[VMEM, VMEM, ANY, VMEM, ANY, ANY, ANY, VMEM, VMEM],
        out_specs=VMEM,
        scratch_shapes=[
            pltpu.VMEM((inner, width), BF16),
            pltpu.VMEM((width, ff), BF16),
            pltpu.VMEM((width, ff), BF16),
            pltpu.VMEM((ff, width), BF16),
            pltpu.VMEM((seqs, width), BF16),
            pltpu.VMEM((seqs, width), BF16),
            pltpu.VMEM((seqs, width), F32),
            pltpu.VMEM((seqs, width), BF16),
            pltpu.VMEM(slots, BF16),
            pltpu.VMEM((n_tp,) + slots, BF16),
            pltpu.VMEM((n_ep * cap, ff), F32),
            pltpu.VMEM((n_ep * cap, ff), F32),
            pltpu.VMEM(slots, BF16),
            pltpu.VMEM(slots, BF16),
            pltpu.VMEM(slots, BF16),
            pltpu.VMEM(slots, BF16),
            pltpu.VMEM(slots, BF16),
            dma((4,)),
            dma((2,)),
            dma((n_ep,)),
            dma((n_ep,)),
            dma((n_ep,)),
            dma((n_ep,)),
            dma((groups,)),
            dma((groups,)),
            dma((n_ep,)),
            dma((n_ep,)),
        ],
        compiler_params=pltpu.CompilerParams(
            collective_id=0, has_side_effects=True, vmem_limit_bytes=48 * 1024 * 1024
        ),
        name="experts",
    )(
        tokens,
        heads_out,
        w_out,
        ffn_gain.reshape(1, width),
        expert_gate,
        expert_up,
        expert_down,
        routes,
        route_weight,
    )
    return (layer_out, new_state)


def solution(mesh):
    in_specs = (
        P("ep", None),
        P(),
        P(None, "tp"),
        P(None, "tp"),
        P(None, "tp"),
        P(None, "tp"),
        P(None, "tp"),
        P(None, "tp"),
        P("tp"),
        P("tp"),
        P("ep", "tp", None, None),
        P(),
        P("tp", None),
        P(),
        P("ep", None, "tp"),
        P("ep", None, "tp"),
        P("ep", "tp", None),
        P("ep", None),
        P("ep", None),
    )
    out_specs = (P("ep", "tp"), P("ep", "tp", None, None))
    body = functools.partial(per_device, mesh.shape["ep"], mesh.shape["tp"])
    return jax.shard_map(body, mesh=mesh, in_specs=in_specs, out_specs=out_specs, check_vma=False)
```

```python
import functools

import jax
import jax.numpy as jnp
from jax import lax
from jax.experimental import pallas as pl
from jax.experimental.pallas import tpu as pltpu
from jax.sharding import PartitionSpec as P

EPS = 1e-06
F32 = jnp.float32
BF16 = jnp.bfloat16
VMEM_LIMIT = 60 * 1024 * 1024
HBM = pl.BlockSpec(memory_space=pltpu.HBM)
VMEM = pl.BlockSpec(memory_space=pltpu.VMEM)


def rms_scale(rows, gain):
    return rows * lax.rsqrt(jnp.mean(rows * rows, axis=-1, keepdims=True) + EPS) * gain


def unit_rows(rows):
    return rows * lax.rsqrt(jnp.sum(rows * rows, axis=-1, keepdims=True) + EPS)


def silu(x):
    return x * jax.nn.sigmoid(x)


def nt_dot(rows, weight):
    return lax.dot_general(rows, weight, (((1,), (1,)), ((), ())), preferred_element_type=F32)


def mixer_kernel(
    step,
    tokens_ref,
    gain_ref,
    wq,
    wk,
    wv,
    wz,
    wd_ref,
    wb_ref,
    rate_ref,
    bias_ref,
    state,
    out_gain_ref,
    heads_out,
    new_state,
    tokens,
    gain,
    wd,
    wb,
    rate,
    bias,
    out_gain,
    small_sem,
    wbuf,
    st,
    ns,
    kq,
    vals,
    zbuf,
    fades,
    betas,
    dots,
    reads,
    w_sem,
    in_sem,
    out_sem,
):
    seqs, heads, dim, _ = st.shape
    chunks = seqs // step

    def w_copy(n):
        return pltpu.make_async_copy((wq, wk, wv, wz)[n], wbuf.at[n], w_sem.at[n])

    def in_copy(c):
        rows = pl.ds(c * step, step)
        return pltpu.make_async_copy(state.at[rows], st.at[rows], in_sem.at[c])

    def out_copy(c):
        rows = pl.ds(c * step, step)
        return pltpu.make_async_copy(ns.at[rows], new_state.at[rows], out_sem.at[c])

    small = [
        pltpu.make_async_copy(src, dst, small_sem.at[n])
        for n, (src, dst) in enumerate(
            (
                (tokens_ref, tokens),
                (gain_ref, gain),
                (wd_ref, wd),
                (wb_ref, wb),
                (rate_ref, rate),
                (bias_ref, bias),
                (out_gain_ref, out_gain),
            )
        )
    ]
    for copy in small:
        copy.start()
    for n in range(4):
        w_copy(n).start()
    for c in range(chunks):
        in_copy(c).start()
    for copy in small:
        copy.wait()

    normed = rms_scale(tokens[...].astype(F32), gain[...]).astype(BF16)

    def rounded(weight):
        return jnp.dot(normed, weight, preferred_element_type=F32).astype(BF16).astype(F32)

    xa = nt_dot(normed, wd[...]).astype(BF16).astype(F32) + bias[...]
    fade = jnp.exp(-rate[...] * (jnp.maximum(xa, 0.0) + jnp.log1p(jnp.exp(-jnp.abs(xa)))))
    beta = jax.nn.sigmoid(nt_dot(normed, wb[...]).astype(BF16).astype(F32))
    for h in range(heads):
        fades[:, h, :] = jnp.broadcast_to(fade[:, h : h + 1], (seqs, dim))
        betas[:, h, :] = jnp.broadcast_to(beta[:, h : h + 1], (seqs, dim))
    w_copy(0).wait()
    raw_q = rounded(wbuf[0])
    w_copy(1).wait()
    raw_k = rounded(wbuf[1])
    for h in range(heads):
        cols = slice(h * dim, (h + 1) * dim)
        query = unit_rows(silu(raw_q[:, cols])) * dim ** (-0.5)
        key = unit_rows(silu(raw_k[:, cols]))
        kq[:, h, :] = key
        kq[:, heads + h, :] = query
        dots[:, h, :] = jnp.broadcast_to(jnp.sum(key * query, axis=-1, keepdims=True), (seqs, dim))
    w_copy(2).wait()
    value = silu(rounded(wbuf[2]))
    for h in range(heads):
        vals[:, h, :] = value[:, h * dim : (h + 1) * dim]
    w_copy(3).wait()
    zbuf[...] = silu(rounded(wbuf[3]))

    def one_chunk(c, carry):
        in_copy(c).wait()
        for i in range(step):
            s = c * step + i
            turned = kq[s].T
            fs, bs, vs, ds = fades[s], betas[s], vals[s], dots[s]
            for h in range(heads):
                block = st[s, h]
                kc = jnp.broadcast_to(turned[:, h : h + 1], (dim, dim))
                qc = jnp.broadcast_to(turned[:, heads + h : heads + h + 1], (dim, dim))
                f = fs[h : h + 1]
                pred = jnp.sum(block * kc, axis=0, keepdims=True)
                proj = jnp.sum(block * qc, axis=0, keepdims=True)
                written = bs[h : h + 1] * (vs[h : h + 1] - f * pred)
                ns[s, h] = f * block + kc * written
                reads[s, pl.ds(h, 1)] = f * proj + written * ds[h : h + 1]
        out_copy(c).start()
        return carry

    lax.fori_loop(0, chunks, one_chunk, 0)
    for h in range(heads):
        cols = slice(h * dim, (h + 1) * dim)
        heads_out[:, cols] = (rms_scale(reads[:, h, :], out_gain[...]) * zbuf[:, cols]).astype(BF16)
    for c in range(chunks):
        out_copy(c).wait()


def expert_kernel(
    n_ep,
    n_tp,
    top,
    cap,
    live,
    groups,
    tokens_ref,
    heads_ref,
    w_out,
    gain_ref,
    w_gate,
    w_up,
    w_down,
    routes_ref,
    weights_ref,
    out,
    tokens,
    heads_out,
    ffn_gain,
    routes,
    weights,
    wo,
    wg,
    wu,
    wdn,
    part_out,
    part_in,
    resid,
    moe,
    disp,
    arrived,
    acc_g,
    acc_u,
    other,
    other_in,
    mine,
    ret_out,
    ret_in,
    w_sem,
    part_sem,
    go_send,
    go_recv,
    fw_send,
    fw_recv,
    half_send,
    half_recv,
    back_send,
    back_recv,
):
    seqs, width = tokens.shape
    cols = width // n_tp
    e = lax.axis_index("ep")
    t = lax.axis_index("tp")
    u = n_tp - 1 - t
    used = pl.ds(0, live)

    def peer(i):
        return lax.rem(e + i, n_ep)

    def source(i):
        return lax.rem(e + n_ep - i, n_ep)

    partner = {"ep": e, "tp": u}
    mesh_ids = pl.DeviceIdType.MESH
    barrier = pltpu.get_barrier_semaphore()
    pl.semaphore_signal(barrier, inc=1, device_id=partner, device_id_type=mesh_ids)

    def greet(i, carry):
        pl.semaphore_signal(barrier, inc=1, device_id={"ep": peer(i), "tp": t}, device_id_type=mesh_ids)
        return carry

    lax.fori_loop(1, n_ep, greet, 0)

    loads = [
        pltpu.make_async_copy(src, dst, w_sem.at[n])
        for n, (src, dst) in enumerate(
            (
                (heads_ref, heads_out),
                (w_out, wo),
                (tokens_ref, tokens),
                (routes_ref, routes),
                (weights_ref, weights),
                (gain_ref, ffn_gain),
                (w_gate.at[0], wg),
                (w_up.at[0], wu),
                (w_down.at[0], wdn),
            )
        )
    ]
    for load in loads:
        load.start()
    for n in (2, 3, 4, 5):
        loads[n].wait()
    eye = lax.broadcasted_iota(jnp.int32, (seqs, seqs), 1) == lax.broadcasted_iota(
        jnp.int32, (seqs, seqs), 0
    )

    def column(row):
        return jnp.sum(jnp.where(eye, row, 0.0), axis=1, keepdims=True)

    lower = (
        lax.broadcasted_iota(jnp.int32, (seqs, seqs), 1)
        < lax.broadcasted_iota(jnp.int32, (seqs, seqs), 0)
    ).astype(BF16)
    picks = []
    taken = jnp.zeros((1, n_ep), F32)
    for j in range(top):
        route = column(routes[j : j + 1, :].astype(F32)).astype(jnp.int32)
        hot = lax.broadcasted_iota(jnp.int32, (seqs, n_ep), 1) == route
        hot_f = hot.astype(F32)
        before = jnp.dot(lower, hot_f.astype(BF16), preferred_element_type=F32) + taken
        slot = jnp.sum(before * hot_f, axis=1, keepdims=True).astype(jnp.int32)
        taken = taken + jnp.sum(hot_f, axis=0, keepdims=True)
        place = route * cap + slot
        picks.append(
            (lax.broadcasted_iota(jnp.int32, (seqs, n_ep * cap), 1) == place).astype(F32)
        )
    spread = sum(picks[1:], picks[0]).T.astype(BF16)

    loads[0].wait()
    loads[1].wait()
    part_out[...] = jnp.dot(heads_out[...], wo[...], preferred_element_type=F32).astype(BF16)
    pl.semaphore_wait(barrier, n_ep)

    swap = pltpu.make_async_remote_copy(
        src_ref=part_out,
        dst_ref=part_in,
        send_sem=part_sem.at[0],
        recv_sem=part_sem.at[1],
        device_id=partner,
        device_id_type=mesh_ids,
    )
    swap.start()
    swap.wait()
    rows = tokens[...].astype(F32) + (part_out[...].astype(F32) + part_in[...].astype(F32))
    resid[...] = rows
    moe[...] = rms_scale(rows, ffn_gain[...]).astype(BF16)
    own = pl.ds(pl.multiple_of(t * cols, 128), cols)
    far = pl.ds(pl.multiple_of(u * cols, 128), cols)
    going = jnp.dot(spread, moe[:, own], preferred_element_type=F32)
    disp[...] = going.reshape(n_ep, cap, cols).astype(BF16)

    def go(i):
        return pltpu.make_async_remote_copy(
            src_ref=disp.at[peer(i), used],
            dst_ref=arrived.at[t, e, used],
            send_sem=go_send.at[i],
            recv_sem=go_recv.at[i],
            device_id={"ep": peer(i), "tp": t},
            device_id_type=mesh_ids,
        )

    def forward(i):
        s = source(i)
        return pltpu.make_async_remote_copy(
            src_ref=arrived.at[t, s, used],
            dst_ref=arrived.at[t, s, used],
            send_sem=fw_send.at[i],
            recv_sem=fw_recv.at[i],
            device_id=partner,
            device_id_type=mesh_ids,
        )

    def go_start(i, carry):
        go(i).start()
        return carry

    lax.fori_loop(1, n_ep, go_start, 0)
    arrived[t, e] = disp[e]
    forward(0).start()

    def pass_on(i, carry):
        go(i).wait_recv()
        forward(i).start()
        return carry

    lax.fori_loop(1, n_ep, pass_on, 0)
    loads[6].wait()
    loads[7].wait()

    def half(which):
        got = arrived[which].astype(F32).reshape(n_ep * cap, cols).astype(BF16)
        part = pl.ds(pl.multiple_of(which * cols, 128), cols)
        return (
            jnp.dot(got, wg[part, :], preferred_element_type=F32),
            jnp.dot(got, wu[part, :], preferred_element_type=F32),
        )

    acc_g[...], acc_u[...] = half(t)

    def fw_done(i, carry):
        forward(i).wait_recv()
        return carry

    lax.fori_loop(0, n_ep, fw_done, 0)
    more_g, more_u = half(u)
    hidden = (silu(acc_g[...] + more_g) * (acc_u[...] + more_u)).astype(BF16)
    loads[8].wait()

    size = n_ep // groups

    def give(g):
        span = pl.ds(g * size, size)
        return pltpu.make_async_remote_copy(
            src_ref=other.at[span],
            dst_ref=other_in.at[span],
            send_sem=half_send.at[g],
            recv_sem=half_recv.at[g],
            device_id=partner,
            device_id_type=mesh_ids,
        )

    def back(s):
        i = lax.rem(e + n_ep - s, n_ep)
        return pltpu.make_async_remote_copy(
            src_ref=ret_out.at[s, used],
            dst_ref=ret_in.at[e, used],
            send_sem=back_send.at[i],
            recv_sem=back_recv.at[i],
            device_id={"ep": s, "tp": t},
            device_id_type=mesh_ids,
        )

    for g in range(groups):
        rows_g = hidden[g * size * cap : (g + 1) * size * cap]
        term = jnp.dot(rows_g, wdn[:, far], preferred_element_type=F32)
        other[pl.ds(g * size, size)] = term.reshape(size, cap, cols).astype(BF16)
        give(g).start()
    term = jnp.dot(hidden, wdn[:, own], preferred_element_type=F32)
    mine[...] = term.reshape(n_ep, cap, cols).astype(BF16)
    for g in range(groups):
        span = pl.ds(g * size, size)
        give(g).wait_recv()
        both = mine[span].astype(F32) + other_in[span].astype(F32)
        ret_out[span] = both.astype(BF16)

        def back_start(s, carry):
            @pl.when(s != e)
            def _():
                back(s).start()

            return carry

        lax.fori_loop(g * size, (g + 1) * size, back_start, 0)
    ret_in[e] = ret_out[e]

    def back_done(i, carry):
        back(source(i)).wait_recv()
        return carry

    lax.fori_loop(1, n_ep, back_done, 0)
    kept = lax.broadcasted_iota(jnp.int32, (n_ep, cap, cols), 1) < live
    returned = jnp.where(kept, ret_in[...].astype(F32), 0.0)
    returned = returned.reshape(n_ep * cap, cols).astype(BF16)
    total = resid[:, own]
    combined = None
    for j in range(top):
        found = jnp.dot(picks[j].astype(BF16), returned, preferred_element_type=F32)
        term = found * column(weights[j : j + 1, :])
        combined = term if combined is None else combined + term
    out[...] = (total + combined).astype(BF16)

    forward(0).wait_send()

    def sent(i, carry):
        go(i).wait_send()
        forward(i).wait_send()
        back(source(i)).wait_send()
        return carry

    lax.fori_loop(1, n_ep, sent, 0)
    for g in range(groups):
        give(g).wait_send()


def per_device(
    n_ep,
    n_tp,
    tokens,
    attn_gain,
    w_query,
    w_key,
    w_value,
    w_zgate,
    w_decay,
    w_beta,
    decay_rate,
    decay_bias,
    state,
    out_gain,
    w_out,
    ffn_gain,
    expert_gate,
    expert_up,
    expert_down,
    routes,
    route_weight,
):
    seqs, width = tokens.shape
    heads, dim = state.shape[1], state.shape[2]
    top = routes.shape[1]
    inner = heads * dim
    step = 2 if seqs % 2 == 0 else 1
    chunks = seqs // step
    heads_out, new_state = pl.pallas_call(
        functools.partial(mixer_kernel, step),
        out_shape=(
            jax.ShapeDtypeStruct((seqs, inner), BF16),
            jax.ShapeDtypeStruct(state.shape, F32),
        ),
        in_specs=[HBM] * 12,
        out_specs=(VMEM, HBM),
        scratch_shapes=[
            pltpu.VMEM((seqs, width), BF16),
            pltpu.VMEM((1, width), F32),
            pltpu.VMEM((heads, width), BF16),
            pltpu.VMEM((heads, width), BF16),
            pltpu.VMEM((1, heads), F32),
            pltpu.VMEM((1, heads), F32),
            pltpu.VMEM((1, dim), F32),
            pltpu.SemaphoreType.DMA((7,)),
            pltpu.VMEM((4, width, inner), BF16),
            pltpu.VMEM(state.shape, F32),
            pltpu.VMEM(state.shape, F32),
            pltpu.VMEM((seqs, 2 * heads, dim), F32),
            pltpu.VMEM((seqs, heads, dim), F32),
            pltpu.VMEM((seqs, inner), F32),
            pltpu.VMEM((seqs, heads, dim), F32),
            pltpu.VMEM((seqs, heads, dim), F32),
            pltpu.VMEM((seqs, heads, dim), F32),
            pltpu.VMEM((seqs, heads, dim), F32),
            pltpu.SemaphoreType.DMA((4,)),
            pltpu.SemaphoreType.DMA((chunks,)),
            pltpu.SemaphoreType.DMA((chunks,)),
        ],
        compiler_params=pltpu.CompilerParams(vmem_limit_bytes=VMEM_LIMIT),
        name="mixer",
    )(
        tokens,
        attn_gain.reshape(1, width),
        w_query,
        w_key,
        w_value,
        w_zgate,
        w_decay.T,
        w_beta.T,
        decay_rate.reshape(1, heads),
        decay_bias.reshape(1, heads),
        state,
        out_gain.reshape(1, dim),
    )

    live = max(2, 2 * seqs * top // n_ep)
    cap = -(-live // 8) * 8
    cols = width // n_tp
    ff = expert_gate.shape[2]
    groups = 4 if n_ep % 4 == 0 else 1
    slots = (n_ep, cap, cols)
    dma = pltpu.SemaphoreType.DMA
    layer_out = pl.pallas_call(
        functools.partial(expert_kernel, n_ep, n_tp, top, cap, live, groups),
        out_shape=jax.ShapeDtypeStruct((seqs, cols), BF16),
        in_specs=[HBM] * 9,
        out_specs=VMEM,
        scratch_shapes=[
            pltpu.VMEM((seqs, width), BF16),
            pltpu.VMEM((seqs, inner), BF16),
            pltpu.VMEM((1, width), F32),
            pltpu.VMEM((top, seqs), jnp.int32),
            pltpu.VMEM((top, seqs), F32),
            pltpu.VMEM((inner, width), BF16),
            pltpu.VMEM((width, ff), BF16),
            pltpu.VMEM((width, ff), BF16),
            pltpu.VMEM((ff, width), BF16),
            pltpu.VMEM((seqs, width), BF16),
            pltpu.VMEM((seqs, width), BF16),
            pltpu.VMEM((seqs, width), F32),
            pltpu.VMEM((seqs, width), BF16),
            pltpu.VMEM(slots, BF16),
            pltpu.VMEM((n_tp,) + slots, BF16),
            pltpu.VMEM((n_ep * cap, ff), F32),
            pltpu.VMEM((n_ep * cap, ff), F32),
            pltpu.VMEM(slots, BF16),
            pltpu.VMEM(slots, BF16),
            pltpu.VMEM(slots, BF16),
            pltpu.VMEM(slots, BF16),
            pltpu.VMEM(slots, BF16),
            dma((9,)),
            dma((2,)),
            dma((n_ep,)),
            dma((n_ep,)),
            dma((n_ep,)),
            dma((n_ep,)),
            dma((groups,)),
            dma((groups,)),
            dma((n_ep,)),
            dma((n_ep,)),
        ],
        compiler_params=pltpu.CompilerParams(
            collective_id=0, has_side_effects=True, vmem_limit_bytes=VMEM_LIMIT
        ),
        name="experts",
    )(
        tokens,
        heads_out,
        w_out,
        ffn_gain.reshape(1, width),
        expert_gate,
        expert_up,
        expert_down,
        routes.T,
        route_weight.T,
    )
    return (layer_out, new_state)


def solution(mesh):
    in_specs = (
        P("ep", None),
        P(),
        P(None, "tp"),
        P(None, "tp"),
        P(None, "tp"),
        P(None, "tp"),
        P(None, "tp"),
        P(None, "tp"),
        P("tp"),
        P("tp"),
        P("ep", "tp", None, None),
        P(),
        P("tp", None),
        P(),
        P("ep", None, "tp"),
        P("ep", None, "tp"),
        P("ep", "tp", None),
        P("ep", None),
        P("ep", None),
    )
    out_specs = (P("ep", "tp"), P("ep", "tp", None, None))
    body = functools.partial(per_device, mesh.shape["ep"], mesh.shape["tp"])
    return jax.shard_map(body, mesh=mesh, in_specs=in_specs, out_specs=out_specs, check_vma=False)
```

```python
import functools

import jax
import jax.numpy as jnp
from jax import lax
from jax.experimental import pallas as pl
from jax.experimental.pallas import tpu as pltpu
from jax.sharding import PartitionSpec as P

EPS = 1e-06
F32 = jnp.float32
BF16 = jnp.bfloat16
VMEM_LIMIT = 60 * 1024 * 1024
HBM = pl.BlockSpec(memory_space=pltpu.HBM)
VMEM = pl.BlockSpec(memory_space=pltpu.VMEM)


def rms_scale(rows, gain):
    return rows * lax.rsqrt(jnp.mean(rows * rows, axis=-1, keepdims=True) + EPS) * gain


def unit_rows(rows):
    return rows * lax.rsqrt(jnp.sum(rows * rows, axis=-1, keepdims=True) + EPS)


def silu(x):
    return x * jax.nn.sigmoid(x)


def nt_dot(rows, weight):
    return lax.dot_general(rows, weight, (((1,), (1,)), ((), ())), preferred_element_type=F32)


def mixer_kernel(
    step,
    tokens_ref,
    gain_ref,
    wq,
    wk,
    wv,
    wz,
    wd_ref,
    wb_ref,
    rate_ref,
    bias_ref,
    state,
    out_gain_ref,
    heads_out,
    new_state,
    tokens,
    gain,
    wd,
    wb,
    rate,
    bias,
    out_gain,
    small_sem,
    wbuf,
    st,
    ns,
    kq,
    vals,
    zbuf,
    fades,
    betas,
    dots,
    reads,
    w_sem,
    in_sem,
    out_sem,
):
    seqs, heads, dim, _ = st.shape
    chunks = seqs // step

    def w_copy(n):
        return pltpu.make_async_copy((wq, wk, wv, wz)[n], wbuf.at[n], w_sem.at[n])

    def in_copy(c):
        rows = pl.ds(c * step, step)
        return pltpu.make_async_copy(state.at[rows], st.at[rows], in_sem.at[c])

    def out_copy(c):
        rows = pl.ds(c * step, step)
        return pltpu.make_async_copy(ns.at[rows], new_state.at[rows], out_sem.at[c])

    small = [
        pltpu.make_async_copy(src, dst, small_sem.at[n])
        for n, (src, dst) in enumerate(
            (
                (tokens_ref, tokens),
                (gain_ref, gain),
                (wd_ref, wd),
                (wb_ref, wb),
                (rate_ref, rate),
                (bias_ref, bias),
                (out_gain_ref, out_gain),
            )
        )
    ]
    for copy in small:
        copy.start()
    for n in range(4):
        w_copy(n).start()
    for c in range(chunks):
        in_copy(c).start()
    for copy in small:
        copy.wait()

    normed = rms_scale(tokens[...].astype(F32), gain[...]).astype(BF16)

    def rounded(weight):
        return jnp.dot(normed, weight, preferred_element_type=F32).astype(BF16).astype(F32)

    xa = nt_dot(normed, wd[...]).astype(BF16).astype(F32) + bias[...]
    fade = jnp.exp(-rate[...] * (jnp.maximum(xa, 0.0) + jnp.log1p(jnp.exp(-jnp.abs(xa)))))
    beta = jax.nn.sigmoid(nt_dot(normed, wb[...]).astype(BF16).astype(F32))
    for h in range(heads):
        fades[:, h, :] = jnp.broadcast_to(fade[:, h : h + 1], (seqs, dim))
        betas[:, h, :] = jnp.broadcast_to(beta[:, h : h + 1], (seqs, dim))
    w_copy(0).wait()
    raw_q = rounded(wbuf[0])
    w_copy(1).wait()
    raw_k = rounded(wbuf[1])
    for h in range(heads):
        cols = slice(h * dim, (h + 1) * dim)
        query = unit_rows(silu(raw_q[:, cols])) * dim ** (-0.5)
        key = unit_rows(silu(raw_k[:, cols]))
        kq[:, h, :] = key
        kq[:, heads + h, :] = query
        dots[:, h, :] = jnp.broadcast_to(jnp.sum(key * query, axis=-1, keepdims=True), (seqs, dim))
    w_copy(2).wait()
    value = silu(rounded(wbuf[2]))
    for h in range(heads):
        vals[:, h, :] = value[:, h * dim : (h + 1) * dim]
    w_copy(3).wait()
    zbuf[...] = silu(rounded(wbuf[3]))

    def one_chunk(c, carry):
        in_copy(c).wait()
        for i in range(step):
            s = c * step + i
            turned = kq[s].T
            fs, bs, vs, ds = fades[s], betas[s], vals[s], dots[s]
            for h in range(heads):
                block = st[s, h]
                kc = jnp.broadcast_to(turned[:, h : h + 1], (dim, dim))
                qc = jnp.broadcast_to(turned[:, heads + h : heads + h + 1], (dim, dim))
                f = fs[h : h + 1]
                pred = jnp.sum(block * kc, axis=0, keepdims=True)
                proj = jnp.sum(block * qc, axis=0, keepdims=True)
                written = bs[h : h + 1] * (vs[h : h + 1] - f * pred)
                ns[s, h] = f * block + kc * written
                reads[s, pl.ds(h, 1)] = f * proj + written * ds[h : h + 1]
        out_copy(c).start()
        return carry

    lax.fori_loop(0, chunks, one_chunk, 0)
    for h in range(heads):
        cols = slice(h * dim, (h + 1) * dim)
        heads_out[:, cols] = (rms_scale(reads[:, h, :], out_gain[...]) * zbuf[:, cols]).astype(BF16)
    for c in range(chunks):
        out_copy(c).wait()


def expert_kernel(
    n_ep,
    n_tp,
    top,
    cap,
    live,
    groups,
    tokens_ref,
    heads_out,
    w_out,
    gain_ref,
    w_gate,
    w_up,
    w_down,
    routes_ref,
    weights_ref,
    out,
    tokens,
    ffn_gain,
    routes,
    weights,
    wo,
    wg,
    wu,
    wdn,
    part_out,
    part_in,
    resid,
    moe,
    disp,
    arrived,
    acc_g,
    acc_u,
    other,
    other_in,
    mine,
    ret_out,
    ret_in,
    w_sem,
    part_sem,
    go_send,
    go_recv,
    fw_send,
    fw_recv,
    half_send,
    half_recv,
    back_send,
    back_recv,
):
    seqs, width = tokens.shape
    cols = width // n_tp
    e = lax.axis_index("ep")
    t = lax.axis_index("tp")
    u = n_tp - 1 - t
    used = pl.ds(0, live)

    def peer(i):
        return lax.rem(e + i, n_ep)

    def source(i):
        return lax.rem(e + n_ep - i, n_ep)

    partner = {"ep": e, "tp": u}
    mesh_ids = pl.DeviceIdType.MESH
    barrier = pltpu.get_barrier_semaphore()
    pl.semaphore_signal(barrier, inc=1, device_id=partner, device_id_type=mesh_ids)

    def greet(i, carry):
        pl.semaphore_signal(barrier, inc=1, device_id={"ep": peer(i), "tp": t}, device_id_type=mesh_ids)
        return carry

    lax.fori_loop(1, n_ep, greet, 0)

    loads = [
        pltpu.make_async_copy(src, dst, w_sem.at[n])
        for n, (src, dst) in enumerate(
            (
                (w_out, wo),
                (tokens_ref, tokens),
                (routes_ref, routes),
                (weights_ref, weights),
                (gain_ref, ffn_gain),
                (w_gate.at[0], wg),
                (w_up.at[0], wu),
                (w_down.at[0], wdn),
            )
        )
    ]
    for load in loads:
        load.start()
    for n in (1, 2, 3, 4):
        loads[n].wait()
    eye = lax.broadcasted_iota(jnp.int32, (seqs, seqs), 1) == lax.broadcasted_iota(
        jnp.int32, (seqs, seqs), 0
    )

    def column(row):
        return jnp.sum(jnp.where(eye, row, 0.0), axis=1, keepdims=True)

    lower = (
        lax.broadcasted_iota(jnp.int32, (seqs, seqs), 1)
        < lax.broadcasted_iota(jnp.int32, (seqs, seqs), 0)
    ).astype(BF16)
    picks = []
    taken = jnp.zeros((1, n_ep), F32)
    for j in range(top):
        route = column(routes[j : j + 1, :].astype(F32)).astype(jnp.int32)
        hot = lax.broadcasted_iota(jnp.int32, (seqs, n_ep), 1) == route
        hot_f = hot.astype(F32)
        before = jnp.dot(lower, hot_f.astype(BF16), preferred_element_type=F32) + taken
        slot = jnp.sum(before * hot_f, axis=1, keepdims=True).astype(jnp.int32)
        taken = taken + jnp.sum(hot_f, axis=0, keepdims=True)
        place = route * cap + slot
        picks.append(
            (lax.broadcasted_iota(jnp.int32, (seqs, n_ep * cap), 1) == place).astype(F32)
        )
    spread = sum(picks[1:], picks[0]).T.astype(BF16)

    loads[0].wait()
    part_out[...] = jnp.dot(heads_out[...], wo[...], preferred_element_type=F32).astype(BF16)
    pl.semaphore_wait(barrier, n_ep)

    swap = pltpu.make_async_remote_copy(
        src_ref=part_out,
        dst_ref=part_in,
        send_sem=part_sem.at[0],
        recv_sem=part_sem.at[1],
        device_id=partner,
        device_id_type=mesh_ids,
    )
    swap.start()
    swap.wait()
    rows = tokens[...].astype(F32) + (part_out[...].astype(F32) + part_in[...].astype(F32))
    resid[...] = rows
    moe[...] = rms_scale(rows, ffn_gain[...]).astype(BF16)
    own = pl.ds(pl.multiple_of(t * cols, 128), cols)
    far = pl.ds(pl.multiple_of(u * cols, 128), cols)
    going = jnp.dot(spread, moe[:, own], preferred_element_type=F32)
    disp[...] = going.reshape(n_ep, cap, cols).astype(BF16)

    def go(i):
        return pltpu.make_async_remote_copy(
            src_ref=disp.at[peer(i), used],
            dst_ref=arrived.at[t, e, used],
            send_sem=go_send.at[i],
            recv_sem=go_recv.at[i],
            device_id={"ep": peer(i), "tp": t},
            device_id_type=mesh_ids,
        )

    def forward(i):
        s = source(i)
        return pltpu.make_async_remote_copy(
            src_ref=arrived.at[t, s, used],
            dst_ref=arrived.at[t, s, used],
            send_sem=fw_send.at[i],
            recv_sem=fw_recv.at[i],
            device_id=partner,
            device_id_type=mesh_ids,
        )

    def go_start(i, carry):
        go(i).start()
        return carry

    lax.fori_loop(1, n_ep, go_start, 0)
    arrived[t, e] = disp[e]
    forward(0).start()

    def pass_on(i, carry):
        go(i).wait_recv()
        forward(i).start()
        return carry

    lax.fori_loop(1, n_ep, pass_on, 0)
    loads[5].wait()
    loads[6].wait()

    def half(which):
        got = arrived[which].astype(F32).reshape(n_ep * cap, cols).astype(BF16)
        part = pl.ds(pl.multiple_of(which * cols, 128), cols)
        return (
            jnp.dot(got, wg[part, :], preferred_element_type=F32),
            jnp.dot(got, wu[part, :], preferred_element_type=F32),
        )

    acc_g[...], acc_u[...] = half(t)

    def fw_done(i, carry):
        forward(i).wait_recv()
        return carry

    lax.fori_loop(0, n_ep, fw_done, 0)
    more_g, more_u = half(u)
    hidden = (silu(acc_g[...] + more_g) * (acc_u[...] + more_u)).astype(BF16)
    loads[7].wait()

    size = n_ep // groups

    def give(g):
        span = pl.ds(g * size, size)
        return pltpu.make_async_remote_copy(
            src_ref=other.at[span],
            dst_ref=other_in.at[span],
            send_sem=half_send.at[g],
            recv_sem=half_recv.at[g],
            device_id=partner,
            device_id_type=mesh_ids,
        )

    def back(s):
        i = lax.rem(e + n_ep - s, n_ep)
        return pltpu.make_async_remote_copy(
            src_ref=ret_out.at[s, used],
            dst_ref=ret_in.at[e, used],
            send_sem=back_send.at[i],
            recv_sem=back_recv.at[i],
            device_id={"ep": s, "tp": t},
            device_id_type=mesh_ids,
        )

    for g in range(groups):
        rows_g = hidden[g * size * cap : (g + 1) * size * cap]
        term = jnp.dot(rows_g, wdn[:, far], preferred_element_type=F32)
        other[pl.ds(g * size, size)] = term.reshape(size, cap, cols).astype(BF16)
        give(g).start()
    term = jnp.dot(hidden, wdn[:, own], preferred_element_type=F32)
    mine[...] = term.reshape(n_ep, cap, cols).astype(BF16)
    for g in range(groups):
        span = pl.ds(g * size, size)
        give(g).wait_recv()
        both = mine[span].astype(F32) + other_in[span].astype(F32)
        ret_out[span] = both.astype(BF16)

        def back_start(s, carry):
            @pl.when(s != e)
            def _():
                back(s).start()

            return carry

        lax.fori_loop(g * size, (g + 1) * size, back_start, 0)
    ret_in[e] = ret_out[e]

    def back_done(i, carry):
        back(source(i)).wait_recv()
        return carry

    lax.fori_loop(1, n_ep, back_done, 0)
    kept = lax.broadcasted_iota(jnp.int32, (n_ep, cap, cols), 1) < live
    returned = jnp.where(kept, ret_in[...].astype(F32), 0.0)
    returned = returned.reshape(n_ep * cap, cols).astype(BF16)
    total = resid[:, own]
    combined = None
    for j in range(top):
        found = jnp.dot(picks[j].astype(BF16), returned, preferred_element_type=F32)
        term = found * column(weights[j : j + 1, :])
        combined = term if combined is None else combined + term
    out[...] = (total + combined).astype(BF16)

    forward(0).wait_send()

    def sent(i, carry):
        go(i).wait_send()
        forward(i).wait_send()
        back(source(i)).wait_send()
        return carry

    lax.fori_loop(1, n_ep, sent, 0)
    for g in range(groups):
        give(g).wait_send()


def per_device(
    n_ep,
    n_tp,
    tokens,
    attn_gain,
    w_query,
    w_key,
    w_value,
    w_zgate,
    w_decay,
    w_beta,
    decay_rate,
    decay_bias,
    state,
    out_gain,
    w_out,
    ffn_gain,
    expert_gate,
    expert_up,
    expert_down,
    routes,
    route_weight,
):
    seqs, width = tokens.shape
    heads, dim = state.shape[1], state.shape[2]
    top = routes.shape[1]
    inner = heads * dim
    step = 2 if seqs % 2 == 0 else 1
    chunks = seqs // step
    heads_out, new_state = pl.pallas_call(
        functools.partial(mixer_kernel, step),
        out_shape=(
            pltpu.VMEM((seqs, inner), BF16),
            jax.ShapeDtypeStruct(state.shape, F32),
        ),
        in_specs=[HBM] * 12,
        out_specs=(VMEM, HBM),
        scratch_shapes=[
            pltpu.VMEM((seqs, width), BF16),
            pltpu.VMEM((1, width), F32),
            pltpu.VMEM((heads, width), BF16),
            pltpu.VMEM((heads, width), BF16),
            pltpu.VMEM((1, heads), F32),
            pltpu.VMEM((1, heads), F32),
            pltpu.VMEM((1, dim), F32),
            pltpu.SemaphoreType.DMA((7,)),
            pltpu.VMEM((4, width, inner), BF16),
            pltpu.VMEM(state.shape, F32),
            pltpu.VMEM(state.shape, F32),
            pltpu.VMEM((seqs, 2 * heads, dim), F32),
            pltpu.VMEM((seqs, heads, dim), F32),
            pltpu.VMEM((seqs, inner), F32),
            pltpu.VMEM((seqs, heads, dim), F32),
            pltpu.VMEM((seqs, heads, dim), F32),
            pltpu.VMEM((seqs, heads, dim), F32),
            pltpu.VMEM((seqs, heads, dim), F32),
            pltpu.SemaphoreType.DMA((4,)),
            pltpu.SemaphoreType.DMA((chunks,)),
            pltpu.SemaphoreType.DMA((chunks,)),
        ],
        compiler_params=pltpu.CompilerParams(vmem_limit_bytes=VMEM_LIMIT),
        name="mixer",
    )(
        tokens,
        attn_gain.reshape(1, width),
        w_query,
        w_key,
        w_value,
        w_zgate,
        w_decay.T,
        w_beta.T,
        decay_rate.reshape(1, heads),
        decay_bias.reshape(1, heads),
        state,
        out_gain.reshape(1, dim),
    )

    live = max(2, 2 * seqs * top // n_ep)
    cap = -(-live // 8) * 8
    cols = width // n_tp
    ff = expert_gate.shape[2]
    groups = 4 if n_ep % 4 == 0 else 1
    slots = (n_ep, cap, cols)
    dma = pltpu.SemaphoreType.DMA
    layer_out = pl.pallas_call(
        functools.partial(expert_kernel, n_ep, n_tp, top, cap, live, groups),
        out_shape=pltpu.VMEM((seqs, cols), BF16),
        in_specs=[HBM, VMEM] + [HBM] * 7,
        out_specs=VMEM,
        scratch_shapes=[
            pltpu.VMEM((seqs, width), BF16),
            pltpu.VMEM((1, width), F32),
            pltpu.VMEM((top, seqs), jnp.int32),
            pltpu.VMEM((top, seqs), F32),
            pltpu.VMEM((inner, width), BF16),
            pltpu.VMEM((width, ff), BF16),
            pltpu.VMEM((width, ff), BF16),
            pltpu.VMEM((ff, width), BF16),
            pltpu.VMEM((seqs, width), BF16),
            pltpu.VMEM((seqs, width), BF16),
            pltpu.VMEM((seqs, width), F32),
            pltpu.VMEM((seqs, width), BF16),
            pltpu.VMEM(slots, BF16),
            pltpu.VMEM((n_tp,) + slots, BF16),
            pltpu.VMEM((n_ep * cap, ff), F32),
            pltpu.VMEM((n_ep * cap, ff), F32),
            pltpu.VMEM(slots, BF16),
            pltpu.VMEM(slots, BF16),
            pltpu.VMEM(slots, BF16),
            pltpu.VMEM(slots, BF16),
            pltpu.VMEM(slots, BF16),
            dma((8,)),
            dma((2,)),
            dma((n_ep,)),
            dma((n_ep,)),
            dma((n_ep,)),
            dma((n_ep,)),
            dma((groups,)),
            dma((groups,)),
            dma((n_ep,)),
            dma((n_ep,)),
        ],
        compiler_params=pltpu.CompilerParams(
            collective_id=0, has_side_effects=True, vmem_limit_bytes=VMEM_LIMIT - 2**21
        ),
        name="experts",
    )(
        tokens,
        pltpu.with_memory_space_constraint(heads_out, pltpu.VMEM),
        w_out,
        ffn_gain.reshape(1, width),
        expert_gate,
        expert_up,
        expert_down,
        routes.T,
        route_weight.T,
    )
    return (layer_out, new_state)


def solution(mesh):
    in_specs = (
        P("ep", None),
        P(),
        P(None, "tp"),
        P(None, "tp"),
        P(None, "tp"),
        P(None, "tp"),
        P(None, "tp"),
        P(None, "tp"),
        P("tp"),
        P("tp"),
        P("ep", "tp", None, None),
        P(),
        P("tp", None),
        P(),
        P("ep", None, "tp"),
        P("ep", None, "tp"),
        P("ep", "tp", None),
        P("ep", None),
        P("ep", None),
    )
    out_specs = (P("ep", "tp"), P("ep", "tp", None, None))
    body = functools.partial(per_device, mesh.shape["ep"], mesh.shape["tp"])
    return jax.shard_map(body, mesh=mesh, in_specs=in_specs, out_specs=out_specs, check_vma=False)
```
